512 devices in a mesh: sp: 64 (over z, y), fs: 4 (over x), tp: 2 (over core).
Axes of the slice: x: 4, y: 8, z: 8, core: 2. Of those that a mesh axis runs over, the one named last changes fastest.
Arguments:
- tokens: bfloat16 [32768, 2048], P(('fs', 'sp')), may hold values from -6 to 6
- in_gain: float32 [2048], replicated, may hold values from 0.1 to 1.9
- query_weight: bfloat16 [2048, 512], P(None, ('tp', 'fs')), may hold values from -0.17291713 to 0.17291713
- key_weight: bfloat16 [2048, 512], P(None, ('tp', 'fs')), may hold values from -0.17291713 to 0.17291713
- value_weight: bfloat16 [2048, 512], P(None, ('tp', 'fs')), may hold values from -0.125 to 0.125
- rec_query_weight: bfloat16 [2048, 512], P(None, ('tp', 'fs')), may hold values from -0.125 to 0.125
- rec_forget_weight: bfloat16 [2048, 512], P(None, ('tp', 'fs')), may hold values from -0.125 to 0.125
- rec_input_weight: bfloat16 [2048, 512], P(None, ('tp', 'fs')), may hold values from -0.125 to 0.125
- mix_lambda: float32 [4], P('tp'), may hold values from 0.3 to 0.8
- lower_bound: float32 [4, 128], P('tp'), may hold values from 0.9 to 0.9999695
- forget_scale: float32 [32768], P(('fs', 'sp')), may hold values from 0.35 to 24576
- att_gain: float32 [128], replicated, may hold values from 0.1 to 1.9
- recurrence_gain: float32 [128], replicated, may hold values from 0.1 to 1.9
- att_out_weight: bfloat16 [512, 2048], P('tp'), may hold values from -0.1875 to 0.1875
- rec_out_weight: bfloat16 [512, 2048], P('tp'), may hold values from -0.1875 to 0.1875
Outputs:
- mixed_out: bfloat16 [32768, 2048], P(('fs', 'sp'))
- log_weight_sum: float32 [4, 32768], P('tp', ('fs', 'sp'))
The draws below stay inside these ranges and needn't reach their ends.
All inputs are finite; a program needn't handle non-finite values.
Results may differ from the reference program's by a relative error of at most 0.012.
Values may be sent and summed in bfloat16 or wider, within the bound.
No kernel may reach another device: no remote copies, remote signals or barrier semaphores. Data moves between devices by JAX's collectives and lax.ppermute only.
A program may use at most 128 MiB of HBM per device.

```python
import math
import jax
import jax.numpy as jnp
from jax import lax

D = 2048
HEADS = 4
DK = 64
DV = 128
BLK = 64
TOK_DEV = 128
LENGTH_PER_SEQ = 8192
SEQS = 4
TOKEN_COUNT_ALL = 32768
N_TP = 2


def drawn_weight(key, salt):
    spread = (D * 10 // 17) ** (-0.5)
    noise = jnp.clip(jax.random.normal(jax.random.fold_in(key, salt), (D, HEADS * 2 * DK), jnp.float32), -4.5, 4.5) * spread
    return jnp.clip(noise, -6.0 * spread, 6.0 * spread).astype(jnp.bfloat16)


def draw_tokens(key, part):
    base = jax.random.normal(jax.random.fold_in(key, 41), (TOKEN_COUNT_ALL, D), jnp.float32)
    return jnp.clip(base, -6.0, 6.0).astype(jnp.bfloat16)


def draw_query_weight(key, part):
    return drawn_weight(key, 51)


def draw_key_weight(key, part):
    return drawn_weight(key, 53)


def draw_lower_bound(key, part):
    first_key, second_key = jax.random.split(jax.random.fold_in(key, 11))
    slower = jax.random.uniform(first_key, (HEADS, DV), jnp.float32) < 0.5
    mixing = jax.random.uniform(second_key, (HEADS, DV), jnp.float32)
    slower_minimum = 0.25 / LENGTH_PER_SEQ
    slow_gap = jnp.exp(math.log(slower_minimum) + mixing * math.log(3.0))
    fast_gap = jnp.exp(math.log(0.04) + mixing * (math.log(0.1) - math.log(0.04)))
    return (1.0 - jnp.where(slower, slow_gap, fast_gap)).astype(jnp.float32)


def draw_forget_scale(key, part):
    key_collection = jax.random.split(jax.random.fold_in(key, 23), 4)
    device_factor = jnp.exp(math.log(0.5) + jax.random.uniform(key_collection[0], (TOKEN_COUNT_ALL // TOK_DEV,), jnp.float32) * math.log(4.0))
    block_factor = jnp.exp(jax.random.uniform(key_collection[1], (TOKEN_COUNT_ALL // BLK,), jnp.float32) * 0.6 - 0.3)
    initial_scale = jnp.repeat(device_factor, TOK_DEV) * jnp.repeat(block_factor, BLK)
    sudden_rows = jax.random.uniform(key_collection[2], (TOKEN_COUNT_ALL,), jnp.float32) < 2.5 / LENGTH_PER_SEQ
    height_per_level = LENGTH_PER_SEQ * (1.0 + 2.0 * jax.random.uniform(key_collection[3], (TOKEN_COUNT_ALL,), jnp.float32))
    return jnp.where(sudden_rows, height_per_level, initial_scale).astype(jnp.float32)


def shard_levels(rng, shape, cuts, least, largest):
    factor_of = 1.0
    for axis_at, shards_of in cuts:
        heights = jax.random.uniform(jax.random.fold_in(jax.random.fold_in(rng, 6), axis_at), (shards_of,), jnp.float32, least / len(cuts), largest / len(cuts))
        factor_of = factor_of * jnp.repeat(jnp.exp(heights), shape[axis_at] // shards_of).reshape((-1,) + (1,) * (len(shape) - 1 - axis_at))
    return factor_of


def bell_draw(rng, extent, scale, reach, cuts=(), kind=jnp.bfloat16):
    values = jax.random.normal(rng, extent, jnp.float32) * scale
    if len(cuts) > 0:
        values = shard_levels(rng, extent, cuts, -0.22, 0.18) * values
    return jnp.clip(values, min=-reach, max=reach).astype(kind)


def setup_inputs(seed: int = 0) -> dict:
    key_of = jax.random.split(jax.random.key(seed), 16)
    return {
        "tokens": draw_tokens(jax.random.fold_in(key_of[15], 71), 0),
        "in_gain": jnp.clip(1.0 + 0.18 * jax.random.normal(key_of[1], (D,), jnp.float32), 0.1, 1.9),
        "query_weight": draw_query_weight(jax.random.fold_in(key_of[15], 71), 0),
        "key_weight": draw_key_weight(jax.random.fold_in(key_of[15], 71), 0),
        "value_weight": bell_draw(key_of[4], (D, HEADS * DV), D ** -0.5, 0.125, ((1, 8),)),
        "rec_query_weight": bell_draw(key_of[5], (D, HEADS * DV), D ** -0.5, 0.125, ((1, 8),)),
        "rec_forget_weight": bell_draw(key_of[6], (D, HEADS * DV), D ** -0.5, 0.125, ((1, 8),)),
        "rec_input_weight": bell_draw(key_of[7], (D, HEADS * DV), D ** -0.5, 0.125, ((1, 8),)),
        "mix_lambda": jnp.clip(0.3 + 0.5 * jax.random.uniform(key_of[8], (HEADS,), jnp.float32) ** shard_levels(key_of[8], (HEADS,), ((0, 2),), -0.2, 0.2), 0.3, 0.8),
        "lower_bound": draw_lower_bound(jax.random.fold_in(key_of[15], 71), 0),
        "forget_scale": draw_forget_scale(jax.random.fold_in(key_of[15], 71), 0),
        "att_gain": jnp.clip(1.0 + 0.18 * jax.random.normal(key_of[11], (DV,), jnp.float32), 0.1, 1.9),
        "recurrence_gain": jnp.clip(1.0 + 0.18 * jax.random.normal(key_of[12], (DV,), jnp.float32), 0.1, 1.9),
        "att_out_weight": bell_draw(key_of[13], (HEADS * DV, D), (2 * HEADS * DV) ** -0.5, 0.1875, ((0, 2),)),
        "rec_out_weight": bell_draw(key_of[14], (HEADS * DV, D), (2 * HEADS * DV) ** -0.5, 0.1875, ((0, 2),)),
    }


EPS = 1e-06
NEG = -1e+30
QUERY_ROWS = 512

def norm_rows(values, gain):
    return values * lax.rsqrt(lax.optimization_barrier(jnp.mean(values * values, axis=-1, keepdims=True)) + EPS) * gain

def to_sequences(rows):
    return rows.reshape(SEQS, LENGTH_PER_SEQ, rows.shape[-1])

def from_sequences(seq_rows):
    return seq_rows.reshape(TOKEN_COUNT_ALL, seq_rows.shape[-1])

def block_recurrence(queries, key_in, value_in, log_forget):
    head_count, row_count, key_width = queries.shape
    block_count = row_count // BLK

    def to_blocks(array_in):
        return array_in.reshape(head_count, block_count, BLK, array_in.shape[-1]).transpose(1, 0, 2, 3)
    causal = jnp.tril(jnp.ones((BLK, BLK), bool))

    def advance(passed_state, inputs):
        query_block, key_block, value_block, l_blk = inputs
        accumulator_sum = jnp.cumsum(l_blk, axis=1)
        cross_block_output = jnp.einsum('sre,sei->sri', query_block * jnp.exp(accumulator_sum), passed_state, precision=lax.Precision.HIGHEST)
        spread = accumulator_sum[:, :, None, :] - accumulator_sum[:, None, :, :]
        decay = jnp.exp(jnp.where(causal[None, :, :, None], spread, -jnp.inf))
        scores = jnp.einsum('htk,htsk,hsk->hts', query_block, decay, key_block, precision=lax.Precision.HIGHEST)
        result = cross_block_output + jnp.einsum('hts,hsv->htv', scores, value_block, precision=lax.Precision.HIGHEST)
        final_log_sum = accumulator_sum[:, -1:, :]
        updated_state = jnp.exp(final_log_sum[:, 0, :])[:, :, None] * passed_state + jnp.einsum('plf,plt->pft', key_block * jnp.exp(final_log_sum - accumulator_sum), value_block, precision=lax.Precision.HIGHEST)
        return (updated_state, result)
    begin_state = jnp.zeros((head_count, key_width, value_in.shape[-1]), jnp.float32)
    end_state, results = lax.scan(advance, begin_state, (to_blocks(queries), to_blocks(key_in), to_blocks(value_in), to_blocks(log_forget)))
    return (end_state, results.transpose(1, 0, 2, 3).reshape(head_count, row_count, value_in.shape[-1]))

def attend_sequence(q_seq, k_seq, v_seq, mix_lambda, att_gain):
    length_now = q_seq.shape[0]
    queries = q_seq.reshape(length_now, HEADS, 2, DK).transpose(1, 2, 0, 3).astype(jnp.float32)
    key_heads = k_seq.reshape(length_now, HEADS, 2, DK).transpose(1, 2, 0, 3).astype(jnp.float32)
    head_values = v_seq.reshape(length_now, HEADS, DV).transpose(1, 0, 2).astype(jnp.float32)
    block_rows = min(QUERY_ROWS, length_now)
    key_pos = jnp.arange(length_now, dtype=jnp.int32)

    def one_block(block_index):
        begin_row = (block_index * block_rows).astype(jnp.int32)
        query_block = lax.dynamic_slice_in_dim(queries, begin_row, block_rows, 2)
        q_pos = begin_row + jnp.arange(block_rows, dtype=jnp.int32)
        allowed = q_pos[:, None] >= key_pos[None, :]
        scores = jnp.einsum('hmqd,hmkd->hmqk', query_block, key_heads) * DK ** (-0.5)
        scores = jnp.where(allowed, scores, NEG)
        highest = lax.optimization_barrier(jnp.max(scores, axis=-1))
        weights = jnp.exp(scores - highest[..., None])
        weight_sum = lax.optimization_barrier(jnp.sum(weights, axis=-1))
        rounded_weights = lax.optimization_barrier(weights.astype(jnp.bfloat16)).astype(jnp.float32)
        summed_values = jnp.einsum('itap,ipn->itan', rounded_weights, head_values)
        mixed = summed_values[:, 0] / weight_sum[:, 0, :, None] - mix_lambda[:, None, None] * summed_values[:, 1] / weight_sum[:, 1, :, None]
        result = (norm_rows(mixed, att_gain) * 0.8).astype(jnp.bfloat16)
        return (result.transpose(1, 0, 2).reshape(block_rows, HEADS * DV), highest[:, 0] + jnp.log(weight_sum[:, 0]))
    results, log_sums = lax.map(one_block, jnp.arange(length_now // block_rows, dtype=jnp.int32))
    return (results.reshape(length_now, HEADS * DV), log_sums.transpose(1, 0, 2).reshape(HEADS, length_now))

def recur_sequence(rq_seq, rf_seq, ri_seq, scale_seq, lower_bound, recurrence_gain):
    length_now = rq_seq.shape[0]

    def heads_first(array_in):
        return array_in.reshape(length_now, HEADS, DV).transpose(1, 0, 2).astype(jnp.float32)
    queries = heads_first(rq_seq)
    lower_edge = lower_bound[:, None, :]
    forget = lower_edge + (1.0 - lower_edge) * jax.nn.sigmoid(heads_first(rf_seq))
    log_forget = scale_seq[None, :, None] * jnp.log(forget)
    key_in = 1.0 - jnp.exp(log_forget)
    _, results = block_recurrence(queries, key_in, heads_first(ri_seq), log_forget)
    normed_out = norm_rows(results, recurrence_gain).astype(jnp.bfloat16)
    return normed_out.transpose(1, 0, 2).reshape(length_now, HEADS * DV)

def reference(tokens, in_gain, query_weight, key_weight, value_weight, rec_query_weight, rec_forget_weight, rec_input_weight, mix_lambda, lower_bound, forget_scale, att_gain, recurrence_gain, att_out_weight, rec_out_weight):
    normed = norm_rows(tokens.astype(jnp.float32), in_gain).astype(jnp.bfloat16)

    def project(weight):
        return to_sequences(jnp.dot(normed, weight, preferred_element_type=jnp.float32).astype(jnp.bfloat16))
    pieces = tuple((project(weight) for weight in (query_weight, key_weight, value_weight, rec_query_weight, rec_forget_weight, rec_input_weight)))
    scales = to_sequences(forget_scale[:, None])[:, :, 0]

    def per_sequence(inputs):
        q_seq, k_seq, v_seq, rq_seq, rf_seq, ri_seq, scale_seq = inputs
        att_rows, log_sums = attend_sequence(q_seq, k_seq, v_seq, mix_lambda, att_gain)
        rec_rows = recur_sequence(rq_seq, rf_seq, ri_seq, scale_seq, lower_bound, recurrence_gain)
        return (att_rows, rec_rows, log_sums)
    att_all, rec_all, log_all = lax.map(per_sequence, pieces + (scales,))
    att_all = from_sequences(att_all)
    rec_all = from_sequences(rec_all)
    log_weight_sum = from_sequences(log_all.transpose(0, 2, 1)).transpose(1, 0)
    group_width = HEADS * DV // N_TP
    mixed = jnp.zeros((TOKEN_COUNT_ALL, D), jnp.float32)
    for group in range(N_TP):
        lower_col = group * group_width
        upper_col = lower_col + group_width
        portion = jnp.dot(att_all[:, lower_col:upper_col], att_out_weight[lower_col:upper_col], preferred_element_type=jnp.float32)
        portion = portion + jnp.dot(rec_all[:, lower_col:upper_col], rec_out_weight[lower_col:upper_col], preferred_element_type=jnp.float32)
        mixed = mixed + lax.optimization_barrier(portion.astype(jnp.bfloat16)).astype(jnp.float32)
    return (mixed.astype(jnp.bfloat16), log_weight_sum)
```

```python
import math

import jax
import jax.numpy as jnp
from jax import lax
from jax.experimental import pallas as pl
from jax.experimental.pallas import tpu as pltpu
from jax.sharding import Mesh
from jax.sharding import PartitionSpec as P

DK = 64
DV = 128
ROWS = 128
HALF = 64
SUB = 16
EPS = 1e-06
NEG = -1e30
LOCAL_HEADS = 2
F32 = jnp.float32
BF16 = jnp.bfloat16
HIGHEST = lax.Precision.HIGHEST

VMEM = pl.BlockSpec(memory_space=pltpu.VMEM)
SMEM = pl.BlockSpec(memory_space=pltpu.SMEM)


def dot(a, b, dims, precision=None):
    return lax.dot_general(a, b, (dims, ((), ())), precision=precision, preferred_element_type=F32)


def dot_nn(a, b, precision=None):
    return dot(a, b, ((1,), (0,)), precision)


def dot_nt(a, b):
    return dot(a, b, ((1,), (1,)))


def dot_tn(a, b):
    return dot(a, b, ((0,), (0,)))


def in_parts(x):
    high = x.astype(BF16).astype(F32)
    rest = x - high
    mid = rest.astype(BF16).astype(F32)
    return high, mid, rest - mid


def rows_to_block(rows, count=16):
    at = lax.broadcasted_iota(jnp.int32, (count, ROWS), 0)
    block = jnp.zeros((count, ROWS), F32)
    for r, row in enumerate(rows):
        block = jnp.where(at == r, row, block)
    return block


def swap_halves(a, b):
    low = lax.broadcasted_iota(jnp.int32, a.shape, 1) < HALF
    first = jnp.where(low, a, pltpu.roll(b, HALF, 1))
    second = jnp.where(low, pltpu.roll(a, HALF, 1), b)
    return first, second


def project_kernel(idx, t0, t1, t2, t3, own, peer, out):
    x, c = idx[2], idx[3]
    rows = jnp.concatenate([t0[...], t1[...], t2[...], t3[...]], axis=0)
    for which, weight in ((c, own), (1 - c, peer)):
        result = dot_nn(rows, weight[...]).astype(BF16)
        for k in range(4):
            seq = lax.rem(x - k + 4, 4)
            out[seq * 2 + which] = result[k * HALF : (k + 1) * HALF]


def gates_kernel(ny, idx, raw, scale, bound, slots, kv_own, decayed_q, local_out):
    width = DV // ny
    y_odd = lax.rem(idx[1], 2) == 1
    row = lax.broadcasted_iota(jnp.int32, (ROWS, ROWS), 0)
    lane = lax.broadcasted_iota(jnp.int32, (ROWS, ROWS), 1)
    lane_sub = lax.broadcasted_iota(jnp.int32, (SUB, ROWS), 1)
    row_sub = lax.broadcasted_iota(jnp.int32, (SUB, ROWS), 0)
    lower = (row >= lane).astype(F32)

    def both(head, offset):
        first = raw[4 * head : 4 * head + 2, :, offset : offset + ROWS].reshape(ROWS, ROWS)
        second = raw[4 * head + 2 : 4 * head + 4, :, offset : offset + ROWS].reshape(ROWS, ROWS)
        return swap_halves(first.astype(F32), second.astype(F32))

    keys, values, ends = [], [], []
    for head in range(LOCAL_HEADS):
        k, v = both(head, 0)
        q, rq = both(head, ROWS)
        rf, ri = both(head, 2 * ROWS)
        keys.append(k)
        values.append(v)
        edge = bound[head : head + 1, :]
        forget = edge + (1.0 - edge) * jax.nn.sigmoid(rf)
        log_forget = scale[...] * jnp.log(forget)
        key_in = 1.0 - jnp.exp(log_forget)
        total = dot_nn(lower, log_forget, HIGHEST)
        end = total[ROWS - 1 : ROWS, :]
        ends.append(end)
        ri16 = ri.astype(BF16)
        state_t = dot_tn(ri16, (key_in * jnp.exp(jnp.minimum(end - total, 0.0))).astype(BF16))
        decayed_q[head] = (rq * jnp.exp(total)).astype(BF16)
        strips = []
        for i in range(ROWS // SUB):
            at = slice(i * SUB, (i + 1) * SUB)
            total_i, rq_i, key_i = total[at], rq[at], key_in[at]
            strip = jnp.zeros((SUB, ROWS), F32)
            if i:
                start = total[i * SUB - 1 : i * SUB]
                far_q = rq_i * jnp.exp(jnp.minimum(total_i - start, 0.0))
                far_k = key_in * jnp.exp(jnp.minimum(start - total, 0.0))
                far = dot_nt(far_q.astype(BF16), far_k.astype(BF16))
                strip = jnp.where(lane_sub < i * SUB, far, strip)
            for s in range(SUB):
                decay = jnp.exp(jnp.minimum(total_i - total_i[s : s + 1], 0.0))
                near = jnp.sum(rq_i * decay * key_i[s : s + 1], axis=1, keepdims=True)
                strip = jnp.where((lane_sub == i * SUB + s) & (row_sub >= s), near, strip)
            strips.append(strip)
        scores = jnp.concatenate(strips, axis=0)
        local_out[head] = dot_nn(scores.astype(BF16), ri16)
        q16, state16 = q.astype(BF16), state_t.astype(BF16)
        for y in range(ny):
            if y % 2 == head:
                slots[y, 0:ROWS, :] = q16
            low = ROWS + head * width
            slots[y, low : low + width, :] = state16[y * width : (y + 1) * width]
    parts = rows_to_block([part for end in ends for part in in_parts(end)]).astype(BF16)
    for y in range(ny):
        slots[y, ROWS + 2 * width : ROWS + 2 * width + 16, :] = parts
    kv_own[0] = jnp.where(y_odd, keys[1], keys[0]).astype(BF16)
    kv_own[1] = jnp.where(y_odd, values[1], values[0]).astype(BF16)


def summed_parts(block, head):
    block = block.astype(F32)
    at = 3 * head
    return block[at : at + 1] + block[at + 1 : at + 2] + block[at + 2 : at + 3]


def prefix_kernel(ny, nz, got, kv_own, kv_peer, out, before, decay):
    width = DV // ny
    first = kv_peer[0].reshape(ROWS, ROWS).astype(F32)
    second = kv_peer[1].reshape(ROWS, ROWS).astype(F32)
    k, v = swap_halves(first, second)
    k16, v16 = k.astype(BF16), v.astype(BF16)
    states, totals = [], []
    for head in range(LOCAL_HEADS):
        state = jnp.zeros((width, ROWS), F32)
        total = jnp.zeros((1, ROWS), F32)
        for y in range(ny):
            before[y, head] = state
            decay[y, head : head + 1, :] = total
            low = ROWS + head * width
            end = summed_parts(got[y, ROWS + 2 * width : ROWS + 2 * width + 16, :], head)
            state = jnp.exp(end) * state + got[y, low : low + width, :].astype(F32)
            total = total + end
        states.append(state.astype(BF16))
        totals.extend(in_parts(total))
    parts = rows_to_block(totals).astype(BF16)
    for z in range(nz):
        out[z, 0:ROWS, :] = kv_own[0]
        out[z, ROWS : 2 * ROWS, :] = k16
        out[z, 2 * ROWS : 3 * ROWS, :] = kv_own[1]
        out[z, 3 * ROWS : 4 * ROWS, :] = v16
        for head in range(LOCAL_HEADS):
            low = 4 * ROWS + head * width
            out[z, low : low + width, :] = states[head]
        out[z, 4 * ROWS + 2 * width : 4 * ROWS + 2 * width + 16, :] = parts


def attend_kernel(ny, nz, idx, got_q, got_kv, before, decay, out, keys, values_t, scores):
    width = DV // ny
    z, y = idx[0], idx[1]
    stats_at = 2 * ROWS
    state_at = stats_at + 16
    for head in range(LOCAL_HEADS):
        entering = jnp.zeros((width, ROWS), F32)
        for k in range(nz):
            end = summed_parts(got_kv[k, 4 * ROWS + 2 * width : 4 * ROWS + 2 * width + 16, :], head)
            low = 4 * ROWS + head * width
            new = jnp.exp(end) * entering + got_kv[k, low : low + width, :].astype(F32)
            entering = jnp.where(k < z, new, entering)
        for k in range(ny):
            low = state_at + head * width
            state = before[k, head] + jnp.exp(decay[k, head : head + 1, :]) * entering
            out[k, low : low + width, :] = state.astype(BF16)

    pair = 2 * ROWS
    for k in range(nz):
        keys[k * pair : (k + 1) * pair, :] = got_kv[k, 0:pair, :]
        for h in range(2):
            block = got_kv[k, pair + h * ROWS : pair + (h + 1) * ROWS, :]
            at = k * pair + h * ROWS
            values_t[:, at : at + ROWS] = block.astype(F32).T.astype(BF16)

    key_row = lax.broadcasted_iota(jnp.int32, (pair, 1), 0)
    other = y + 1 - 2 * lax.rem(y, 2)
    key_at = jnp.where(key_row < ROWS, y * ROWS + key_row, other * ROWS + key_row - ROWS)
    query_lane = lax.broadcasted_iota(jnp.int32, (1, pair), 1)
    low_lanes = lax.broadcasted_iota(jnp.int32, (pair, ROWS), 1) < HALF
    scale = DK ** (-0.5)
    for group in range(ny // 2):
        q = jnp.concatenate([got_q[2 * group, 0:ROWS, :], got_q[2 * group + 1, 0:ROWS, :]], axis=0)
        q = q.astype(F32) * scale
        query_at = z * (ny * ROWS) + group * pair + query_lane
        stats = []
        for m in range(2):
            q_map = jnp.where(low_lanes == (m == 0), q, 0.0).astype(BF16)
            highest = jnp.full((8, pair), NEG, F32)
            for k in range(nz):
                part = dot_nt(keys[k * pair : (k + 1) * pair, :], q_map)
                part = jnp.where(key_at + k * (ny * ROWS) <= query_at, part, NEG)
                scores[k * pair : (k + 1) * pair, :] = part
                highest = jnp.maximum(highest, jnp.max(part.reshape(pair // 8, 8, pair), axis=0))
            top = jnp.max(highest, axis=0, keepdims=True)
            summed = jnp.zeros((8, pair), F32)
            numer = jnp.zeros((DV, pair), F32)
            for k in range(nz):
                weights = jnp.exp(scores[k * pair : (k + 1) * pair, :] - top)
                summed = summed + jnp.sum(weights.reshape(pair // 8, 8, pair), axis=0)
                numer = numer + dot_nn(
                    values_t[:, k * pair : (k + 1) * pair], weights.astype(BF16)
                )
            weight_sum = jnp.sum(summed, axis=0, keepdims=True)
            numer = (numer * (1.0 / weight_sum)).astype(BF16)
            stats.append(in_parts(top + jnp.log(weight_sum)))
            for h in range(2):
                cut = slice(h * ROWS, (h + 1) * ROWS)
                out[2 * group + h, m * ROWS : (m + 1) * ROWS, :] = numer[:, cut]
        for h in range(2):
            cut = slice(h * ROWS, (h + 1) * ROWS)
            block = rows_to_block([part[:, cut] for parts in stats for part in parts])
            out[2 * group + h, stats_at : stats_at + 16, :] = block.astype(BF16)


def combine_kernel(
    ny, mix, got, decayed_q, local_out, att_gain, rec_gain, w_att, w_rec, partial, log_sum
):
    width = DV // ny
    stats_at = 2 * ROWS
    state_at = stats_at + 16
    att_heads, rec_heads = [], []
    for head in range(LOCAL_HEADS):
        sources = [k for k in range(ny) if k % 2 == head]
        maps = []
        for m in range(2):
            logs = [summed_parts(got[k, stats_at : stats_at + 16, :], m) for k in sources]
            top = logs[0]
            for entry in logs[1:]:
                top = jnp.maximum(top, entry)
            shares = [jnp.exp(entry - top) for entry in logs]
            total = shares[0]
            for share in shares[1:]:
                total = total + share
            if m == 0:
                log_sum[head : head + 1, :] = top + jnp.log(total)
            inverse = 1.0 / total
            merged = jnp.zeros((DV, ROWS), F32)
            for k, share in zip(sources, shares):
                numer = got[k, m * ROWS : (m + 1) * ROWS, :].astype(F32)
                merged = merged + numer * (share * inverse)
            maps.append(merged)
        att = maps[0] - mix[head] * maps[1]
        att = att * lax.rsqrt(jnp.mean(att * att, axis=0, keepdims=True) + EPS)
        att_heads.append((att.T * att_gain[...] * 0.8).astype(BF16))
        low = state_at + head * width
        state_t = jnp.concatenate([got[k, low : low + width, :] for k in range(ny)], axis=0)
        rec = local_out[head] + dot_nt(decayed_q[head], state_t)
        rec = rec * lax.rsqrt(jnp.mean(rec * rec, axis=1, keepdims=True) + EPS)
        rec_heads.append((rec * rec_gain[...]).astype(BF16))
    att_rows = jnp.concatenate(att_heads, axis=1)
    rec_rows = jnp.concatenate(rec_heads, axis=1)
    result = dot_nn(att_rows, w_att[...]) + dot_nn(rec_rows, w_rec[...])
    partial[...] = result.astype(BF16)


def ring(size, step):
    return [(i, (i + step) % size) for i in range(size)]


def on_device(ny, nz, *args):
    (tokens, in_gain, wq, wk, wv, wrq, wrf, wri, mix_lambda, lower_bound) = args[:10]
    (forget_scale, att_gain, recurrence_gain, att_out_weight, rec_out_weight) = args[10:]
    z, y, x, c = (lax.axis_index(name) for name in ("z", "y", "x", "c"))
    idx = jnp.stack([z, y, x, c]).astype(jnp.int32)
    width = DV // ny
    d_model = tokens.shape[1]

    rows = lax.dynamic_slice_in_dim(tokens, c * HALF, HALF, 0).astype(F32)
    mean_square = jnp.mean(rows * rows, axis=-1, keepdims=True)
    normed = (rows * lax.rsqrt(mean_square + EPS) * in_gain).astype(BF16)
    gathered = [normed] + [lax.ppermute(normed, "x", ring(4, k)) for k in (1, 2, 3)]
    own = jnp.concatenate([wk, wv, wq, wrq, wrf, wri], axis=1)
    peer = lax.ppermute(own, "c", ring(2, 1))

    projected = pl.pallas_call(
        project_kernel,
        out_shape=jax.ShapeDtypeStruct((8, HALF, 384), BF16),
        in_specs=[SMEM] + [VMEM] * 6,
        out_specs=VMEM,
        name="project",
    )(idx, *gathered, own, peer)
    raw = lax.all_to_all(projected, ("x", "c"), 0, 0, tiled=True)

    other_head = 1 - lax.rem(y, 2)
    kv_send = lax.dynamic_slice(
        raw.reshape(4, 2, HALF, 384), (2 * other_head, 0, 0, 0), (2, 2, HALF, ROWS)
    )
    kv_peer = lax.ppermute(kv_send, "y", [(i, i ^ 1) for i in range(ny)])

    slots, kv_own, decayed_q, local_out = pl.pallas_call(
        lambda *refs: gates_kernel(ny, *refs),
        out_shape=(
            jax.ShapeDtypeStruct((ny, ROWS + 2 * width + 16, ROWS), BF16),
            jax.ShapeDtypeStruct((2, ROWS, ROWS), BF16),
            jax.ShapeDtypeStruct((LOCAL_HEADS, ROWS, ROWS), BF16),
            jax.ShapeDtypeStruct((LOCAL_HEADS, ROWS, ROWS), F32),
        ),
        in_specs=[SMEM, VMEM, VMEM, VMEM],
        out_specs=(VMEM,) * 4,
        name="gates",
    )(idx, raw, forget_scale.reshape(ROWS, 1), lower_bound)
    got_q = lax.all_to_all(slots, "y", 0, 0, tiled=True)

    kv_slots, before, decay = pl.pallas_call(
        lambda *refs: prefix_kernel(ny, nz, *refs),
        out_shape=(
            jax.ShapeDtypeStruct((nz, 4 * ROWS + 2 * width + 16, ROWS), BF16),
            jax.ShapeDtypeStruct((ny, LOCAL_HEADS, width, ROWS), F32),
            jax.ShapeDtypeStruct((ny, LOCAL_HEADS, ROWS), F32),
        ),
        in_specs=[VMEM] * 3,
        out_specs=(VMEM,) * 3,
        name="prefix",
    )(got_q, kv_own, kv_peer)
    got_kv = lax.all_to_all(kv_slots, "z", 0, 0, tiled=True)

    keys_in_all = nz * 2 * ROWS
    results = pl.pallas_call(
        lambda *refs: attend_kernel(ny, nz, *refs),
        out_shape=jax.ShapeDtypeStruct((ny, 2 * ROWS + 16 + 2 * width, ROWS), BF16),
        in_specs=[SMEM] + [VMEM] * 4,
        out_specs=VMEM,
        scratch_shapes=[
            pltpu.VMEM((keys_in_all, ROWS), BF16),
            pltpu.VMEM((DV, keys_in_all), BF16),
            pltpu.VMEM((keys_in_all, 2 * ROWS), F32),
        ],
        name="attend",
    )(idx, got_q, got_kv, before, decay)
    returned = lax.all_to_all(results, "y", 0, 0, tiled=True)

    partial, log_weight_sum = pl.pallas_call(
        lambda *refs: combine_kernel(ny, *refs),
        out_shape=(
            jax.ShapeDtypeStruct((ROWS, d_model), BF16),
            jax.ShapeDtypeStruct((LOCAL_HEADS, ROWS), F32),
        ),
        in_specs=[SMEM] + [VMEM] * 7,
        out_specs=(VMEM, VMEM),
        name="combine",
    )(
        mix_lambda,
        returned,
        decayed_q,
        local_out,
        att_gain.reshape(1, DV),
        recurrence_gain.reshape(1, DV),
        att_out_weight,
        rec_out_weight,
    )
    other = lax.ppermute(partial, "c", ring(2, 1))
    mixed_out = (partial.astype(F32) + other.astype(F32)).astype(BF16)
    return mixed_out, log_weight_sum


def solution(mesh):
    side = math.isqrt(mesh.shape["sp"])
    finer = Mesh(
        mesh.devices.reshape(side, side, mesh.shape["fs"], mesh.shape["tp"]), ("z", "y", "x", "c")
    )
    rows = ("x", "z", "y")
    columns = P(None, ("c", "x"))
    placed = (P(rows, None), P()) + (columns,) * 6
    placed += (P("c"), P("c", None), P(rows), P(), P(), P("c", None), P("c", None))
    return jax.shard_map(
        lambda *args: on_device(side, side, *args),
        mesh=finer,
        in_specs=placed,
        out_specs=(P(rows, None), P("c", rows)),
        check_vma=False,
    )
```
